32 devices in a mesh: ep: 8 (over z, core), tp: 4 (over y, x).
Axes of the slice: x: 2, y: 2, z: 4, core: 2. Of those that a mesh axis runs over, the one named last changes fastest.
Arguments:
- mixer_rows: bfloat16 [4096, 2048], P('ep', 'tp'), may hold values from -6 to 6
- expert_rows: bfloat16 [4096, 2048], P('ep', 'tp'), may hold values from -6 to 6
- mixer_gain: float32 [2048], replicated, may hold values from 0.1 to 1.9
- pool_scale: float32 [2048], P('tp'), may hold values from 0.1 to 1.9
- w_in: bfloat16 [2048, 2048], P(None, 'tp'), may hold values from -0.125 to 0.125
- w_mix_out: bfloat16 [2048, 2048], P(None, 'tp'), may hold values from -0.125 to 0.125
- expert_gain: float32 [2048], replicated, may hold values from 0.1 to 1.9
- expert_gate: bfloat16 [8, 2048, 2048], P('ep', None, 'tp'), may hold values from -0.125 to 0.125
- expert_up: bfloat16 [8, 2048, 2048], P('ep', None, 'tp'), may hold values from -0.125 to 0.125
- expert_down: bfloat16 [8, 2048, 2048], P('ep', None, 'tp'), may hold values from -0.125 to 0.125
- routes: int32 [4096, 2], P('ep'), may hold values from 0 to 7, all different within a row; in each aligned block of 512 rows (0 to 511, 512 to 1023, ...) at most 192 rows name the same one
- route_weight: float32 [4096, 2], P('ep'), may hold values from 0.1 to 1
Outputs:
- mixer_output: bfloat16 [4096, 2048], P('ep', 'tp')
- expert_output: bfloat16 [4096, 2048], P('ep', 'tp')
The draws below stay inside these ranges and needn't reach their ends.
Inputs may be any that keep to these rules, and one draw needn't show every extreme that they name: `routes`: each row names 2 different experts. Among the rows of one device (aligned blocks of 512 rows) no expert is named more than 192 times, a bound that some block reaches.
All inputs are finite; a program needn't handle non-finite values.
Results may differ from the reference program's by a relative error of at most 0.0071.
Values may be sent and summed in bfloat16 or wider, within the bound.
A program may use at most 64 MiB of HBM per device.

```python
import math
import jax
import jax.numpy as jnp
import numpy as np
from jax import lax

D = 2048
PW = 2048
FE = 2048
TOP = 2
TOK_DEV = 512
TOKENS = 4096
EXPERTS = 8
CAP = 192
N_EP = 8


def steps_of(own_key, dims, pieces, smallest, top_value):
    def one(axis_at, parts):
        draws = jax.random.uniform(jax.random.fold_in(jax.random.fold_in(own_key, 6), axis_at), (parts,), jnp.float32, smallest / len(pieces), top_value / len(pieces))
        return jnp.repeat(jnp.exp(draws), dims[axis_at] // parts).reshape((-1,) + (1,) * (len(dims) - axis_at - 1))

    loudness = one(*pieces[0])
    for cut in pieces[1:]:
        loudness = loudness * one(*cut)
    return loudness


def shared_out(key, own, number, rows, amount, top, most, skew):
    sequence = jax.random.permutation(key, amount)
    crowded, common = portions_of(amount, rows * top, most, skew, True), portions_of(amount, rows * top, most, skew, False)
    places = jnp.arange(amount)

    def named(tallies, turn):
        used = int((tallies > 0).sum())
        fixed = max(1, used // 4)
        moved = fixed + (places - fixed + turn * (used - fixed)) % max(1, amount - fixed)
        return jnp.zeros((amount,), jnp.int32).at[sequence[jnp.where(places < fixed, places, moved)]].set(jnp.asarray(tallies, jnp.int32))

    tallies = jnp.where(number % 4 == 0, named(crowded, number // 4), named(common, number - number // 4 - 1))
    mixed = jax.random.permutation(jax.random.fold_in(own, 3), amount)
    donor, sink = mixed[0:amount // 2 * 2:2], mixed[1:amount // 2 * 2:2]
    room = jnp.minimum(tallies[donor] - 1, most - tallies[sink]) // 2
    room = jnp.where((donor == sequence[0]) | (sink == sequence[0]) | (tallies[sink] == 0), 0, jnp.maximum(room, 0))
    moved = jax.random.randint(jax.random.fold_in(own, 4), (amount // 2,), 0, 1 << 20) % (room + 1)
    tallies = tallies.at[donor].add(-moved).at[sink].add(moved)
    members = jnp.searchsorted(jnp.cumsum(tallies), jnp.arange(rows * top), side="right").astype(jnp.int32)
    listing = members.reshape(top, rows).T
    listing = listing[jax.random.permutation(jax.random.fold_in(own, 1), rows)]
    turn = jax.random.randint(jax.random.fold_in(own, 2), (rows, 1), 0, top)
    return jnp.take_along_axis(listing, (jnp.arange(top)[None, :] + turn) % top, axis=1)


def portions_of(count, total, reach, slope, full):
    loads = [(1 << 20) // math.isqrt(grade ** slope) + 1 for grade in range(1, count + 1)]
    largest = reach if full else min(reach, max(-(-total // count), total * loads[0] // sum(loads)))
    least = 1 if total - largest >= count - 1 else 0
    holding, rest = [largest] + [least] * (count - 1), total - largest - least * (count - 1)
    while rest > 0:
        movable = [i for i in range(1, count) if holding[i] < largest] or [i for i in range(1, count) if holding[i] < reach]
        pool, remaining = sum([loads[i] for i in movable]), rest
        for i in movable:
            extra = min(reach - holding[i], max(1, remaining * loads[i] // pool), rest)
            holding[i] = holding[i] + extra
            rest = rest - extra
    return np.array(holding)


def gaussian(stream_key, extent, deviation, most, shards=(), kind=jnp.bfloat16):
    entries = jax.random.normal(stream_key, extent, jnp.float32) * deviation
    if len(shards) > 0:
        entries = steps_of(stream_key, extent, shards, -0.22, 0.18) * entries
    return jnp.clip(entries, min=-most, max=most).astype(kind)


def setup_inputs(seed: int = 0) -> dict:
    key_list = jax.random.split(jax.random.key(seed), 13)
    mixer_rows = gaussian(key_list[0], (TOKENS, D), 1.0, 6.0, ((0, 8), (1, 4)))
    expert_rows = gaussian(key_list[1], (TOKENS, D), 1.0, 6.0, ((0, 8), (1, 4)))
    mixer_gain = jnp.clip(1.0 + 0.18 * jax.random.normal(key_list[2], (D,), jnp.float32), 0.1, 1.9)
    pool_scale = jnp.clip(1.0 + 0.18 * jax.random.normal(key_list[3], (PW,), jnp.float32), 0.1, 1.9)
    w_in = gaussian(key_list[4], (D, PW), D ** -0.5, 0.125, ((1, 4),))
    w_mix_out = gaussian(key_list[5], (PW, D), PW ** -0.5, 0.125, ((1, 4),))
    expert_gain = jnp.clip(1.0 + 0.18 * jax.random.normal(key_list[6], (D,), jnp.float32), 0.1, 1.9)
    expert_gate = gaussian(key_list[7], (EXPERTS, D, FE), D ** -0.5, 0.125, ((0, 8), (2, 4)))
    expert_up = gaussian(key_list[8], (EXPERTS, D, FE), D ** -0.5, 0.125, ((0, 8), (2, 4)))
    expert_down = gaussian(key_list[9], (EXPERTS, FE, D), FE ** -0.5, 0.125, ((0, 8), (2, 4)))
    routes_keys = jax.random.split(jax.random.fold_in(key_list[10], 1), TOKENS // TOK_DEV)
    routes_turns = jax.random.permutation(jax.random.fold_in(key_list[10], 3), TOKENS // TOK_DEV)
    routes = jax.vmap(lambda own, number: shared_out(jax.random.fold_in(key_list[10], 2), own, number, TOK_DEV, EXPERTS, TOP, CAP, 1))(routes_keys, routes_turns).reshape((TOKENS, TOP))
    route_weight = jnp.clip(jnp.exp(math.log(1.0) - 2.3025851 * jax.random.uniform(key_list[11], (TOKENS, TOP), jnp.float32) ** steps_of(key_list[11], (TOKENS, TOP), ((0, 8),), -0.2, 0.2)), 0.1, 1.0)
    return {"mixer_rows": mixer_rows, "expert_rows": expert_rows, "mixer_gain": mixer_gain, "pool_scale": pool_scale, "w_in": w_in, "w_mix_out": w_mix_out, "expert_gain": expert_gain, "expert_gate": expert_gate, "expert_up": expert_up, "expert_down": expert_down, "routes": routes, "route_weight": route_weight}


norm_eps = 1e-05
pool_windows = (2, 4, 8, 16)

def layer_norm(row_block, gain_vec):
    values = row_block.astype(jnp.float32)
    center = values - lax.optimization_barrier(jnp.mean(values, axis=-1, keepdims=True))
    spread = lax.optimization_barrier(jnp.mean(center * center, axis=-1, keepdims=True))
    return (center * lax.rsqrt(spread + norm_eps) * gain_vec).astype(jnp.bfloat16)

def reference(mixer_rows, expert_rows, mixer_gain, pool_scale, w_in, w_mix_out, expert_gain, expert_gate, expert_up, expert_down, routes, route_weight):
    normed_mix = layer_norm(mixer_rows, mixer_gain)
    inner_proj = jnp.dot(normed_mix, w_in, preferred_element_type=jnp.float32).astype(jnp.bfloat16)
    values = inner_proj.astype(jnp.float32)
    seq_len = values.shape[0]
    prefix = jnp.concatenate([jnp.zeros((1, PW), jnp.float32), jnp.cumsum(values, axis=0)], axis=0)
    position = jnp.arange(seq_len, dtype=jnp.int32)
    group_width = PW // 4
    window_means = []
    for group_id, window in enumerate(pool_windows):
        lower_end = jnp.clip(position - window // 2, 0, seq_len)
        upper_end = jnp.clip(position - window // 2 + window, 0, seq_len)
        counts = (upper_end - lower_end).astype(jnp.float32)[:, None]
        columns = prefix[:, group_id * group_width:(group_id + 1) * group_width]
        window_means.append((columns[upper_end] - columns[lower_end]) / counts)
    pooled = ((jnp.concatenate(window_means, axis=1) - values) * pool_scale).astype(jnp.bfloat16)
    mixer_output = jnp.dot(pooled, w_mix_out, preferred_element_type=jnp.float32).astype(jnp.bfloat16)
    normed_expert = layer_norm(expert_rows, expert_gain)
    flat_route = routes.reshape(-1).astype(jnp.int32)
    onehot = (flat_route[:, None] == jnp.arange(EXPERTS, dtype=jnp.int32)[None, :]).astype(jnp.int32)
    running = jnp.cumsum(onehot.reshape(N_EP, TOK_DEV * TOP, EXPERTS), axis=1).reshape(-1, EXPERTS)
    ranking = lax.optimization_barrier(jnp.sum(onehot * (running - 1), axis=1))
    source_dev = jnp.arange(TOKENS * TOP, dtype=jnp.int32) // (TOK_DEV * TOP)
    slot_index = (flat_route * N_EP + source_dev) * CAP + ranking
    token_index = jnp.arange(TOKENS * TOP, dtype=jnp.int32) // TOP
    slot_table = jnp.zeros((EXPERTS * N_EP * CAP, D), jnp.bfloat16).at[slot_index].set(normed_expert[token_index])

    def run_expert(packed):
        slot_rows, gate_weight, up_weight, down_weight = packed
        gate_val = jnp.dot(slot_rows, gate_weight, preferred_element_type=jnp.float32)
        up_val = jnp.dot(slot_rows, up_weight, preferred_element_type=jnp.float32)
        hidden = (jax.nn.silu(gate_val) * up_val).astype(jnp.bfloat16)
        return jnp.dot(hidden, down_weight, preferred_element_type=jnp.float32).astype(jnp.bfloat16)
    results = lax.map(run_expert, (slot_table.reshape(EXPERTS, N_EP * CAP, D), expert_gate, expert_up, expert_down))
    picked = results.reshape(-1, D)[slot_index].astype(jnp.float32).reshape(TOKENS, TOP, D)
    expert_output = lax.optimization_barrier(jnp.sum(picked * route_weight[:, :, None], axis=1)).astype(jnp.bfloat16)
    return (mixer_output, expert_output)
```

```python
import functools

import jax
import jax.numpy as jnp
from jax import lax
from jax.experimental import pallas as pl
from jax.experimental.pallas import tpu as pltpu
from jax.sharding import PartitionSpec as P

TOP = 2
norm_eps = 1e-05
pool_windows = (2, 4, 8, 16)
RIM = 16
MESH = pl.DeviceIdType.MESH
f32 = jnp.float32
bf16 = jnp.bfloat16


def fused(
    ep,
    tp,
    xm_in,
    xe_in,
    gain_m,
    gain_e,
    scale,
    trow,
    tcol,
    rw,
    w_in_h,
    w_mix_h,
    gate_h,
    up_h,
    down_h,
    out_m,
    out_e,
    w_in,
    w_mix,
    gate,
    up,
    down,
    xm,
    xe,
    normed,
    disp_send,
    disp_recv,
    hid,
    pooled,
    back_send,
    back_recv,
    ext,
    rim_send,
    rim_recv,
    acc,
    w_sem,
    xe_s,
    xe_r,
    xm_s,
    xm_r,
    dp_s,
    dp_r,
    rim_s,
    rim_r,
    po_s,
    po_r,
    hi_s,
    hi_r,
    bk_s,
    bk_r,
):
    me_ep = lax.axis_index("ep")
    me_tp = lax.axis_index("tp")
    rows, feat = xm_in.shape
    cap = disp_recv.shape[1]
    chan = out_m.shape[1]
    width = feat * tp
    chunk = min(rows, 128)

    barrier = pltpu.get_barrier_semaphore()
    for d in range(1, tp):
        pl.semaphore_signal(
            barrier, inc=1, device_id={"tp": lax.rem(me_tp + d, tp)}, device_id_type=MESH
        )
    for d in range(1, ep):
        pl.semaphore_signal(
            barrier, inc=1, device_id={"ep": lax.rem(me_ep + d, ep)}, device_id_type=MESH
        )
    pl.semaphore_wait(barrier, tp + ep - 2)

    def tp_copy(src, dst, s, r, d):
        return pltpu.make_async_remote_copy(
            src_ref=src,
            dst_ref=dst,
            send_sem=s,
            recv_sem=r,
            device_id={"tp": lax.rem(me_tp + d, tp)},
            device_id_type=MESH,
        )

    def ep_copy(src, dst, s, r, d):
        return pltpu.make_async_remote_copy(
            src_ref=src,
            dst_ref=dst,
            send_sem=s,
            recv_sem=r,
            device_id={"ep": lax.rem(me_ep + d, ep)},
            device_id_type=MESH,
        )

    def tp_from(d):
        return lax.rem(me_tp - d + tp, tp)

    def ep_from(d):
        return lax.rem(me_ep - d + ep, ep)

    for d in range(1, tp):
        tp_copy(xe_in, xe.at[me_tp], xe_s.at[d - 1], xe_r.at[d - 1], d).start()
    for d in range(1, tp):
        tp_copy(xm_in, xm.at[me_tp], xm_s.at[d - 1], xm_r.at[d - 1], d).start()

    loads = [
        pltpu.make_async_copy(h, v, w_sem.at[i])
        for i, (h, v) in enumerate(
            ((w_in_h, w_in), (gate_h, gate), (up_h, up), (w_mix_h, w_mix), (down_h, down))
        )
    ]
    for load in loads:
        load.start()

    xe[me_tp] = xe_in[...]
    xm[me_tp] = xm_in[...]

    def norm_into(gathered, gain):
        def step(i, carry):
            at = pl.ds(pl.multiple_of(i * chunk, chunk), chunk)
            parts = [gathered[p, at, :].astype(f32) for p in range(tp)]
            total = sum(jnp.sum(v, axis=-1, keepdims=True) for v in parts)
            mean = total / width
            parts = [v - mean for v in parts]
            spread = sum(jnp.sum(v * v, axis=-1, keepdims=True) for v in parts) / width
            inv = lax.rsqrt(spread + norm_eps)
            for p in range(tp):
                cols = slice(p * feat, (p + 1) * feat)
                normed[at, cols] = (parts[p] * inv * gain[:, cols]).astype(bf16)
            return carry

        lax.fori_loop(0, rows // chunk, step, 0)

    for d in range(1, tp):
        tp_copy(xe_in, xe.at[tp_from(d)], xe_s.at[d - 1], xe_r.at[d - 1], d).wait_recv()
    norm_into(xe, gain_e)

    def picked_rows(e):
        slot = lax.broadcasted_iota(jnp.int32, (cap, rows), 0) + e * cap
        hit = (slot == trow[0:1, :]) | (slot == trow[1:2, :])
        pick = jnp.where(hit, 1.0, 0.0).astype(bf16)
        return jnp.dot(pick, normed[...], preferred_element_type=f32).astype(bf16)

    def send_rows(d, carry):
        e = lax.rem(me_ep + d, ep)
        disp_send[e] = picked_rows(e)
        ep_copy(disp_send.at[e], disp_recv.at[me_ep], dp_s.at[d], dp_r.at[d], d).start()
        return carry

    lax.fori_loop(1, ep, send_rows, 0)
    disp_recv[me_ep] = picked_rows(me_ep)

    for d in range(1, tp):
        tp_copy(xm_in, xm.at[tp_from(d)], xm_s.at[d - 1], xm_r.at[d - 1], d).wait_recv()
    norm_into(xm, gain_m)
    loads[0].wait()

    def project(i, carry):
        at = pl.ds(pl.multiple_of(i * chunk, chunk), chunk)
        inner = jnp.dot(normed[at, :], w_in[...], preferred_element_type=f32).astype(bf16)
        ext[pl.ds(pl.multiple_of(RIM + i * chunk, RIM), chunk), :] = inner.astype(f32)
        return carry

    lax.fori_loop(0, rows // chunk, project, 0)
    rim_send[0] = ext[rows : rows + RIM, :].astype(bf16)
    rim_send[1] = ext[RIM : 2 * RIM, :].astype(bf16)
    up_rim = ep_copy(rim_send.at[0], rim_recv.at[0], rim_s.at[0], rim_r.at[0], 1)
    down_rim = ep_copy(rim_send.at[1], rim_recv.at[1], rim_s.at[1], rim_r.at[1], ep - 1)
    up_rim.start()
    down_rim.start()

    loads[1].wait()
    loads[2].wait()

    def hidden_of(q):
        x = disp_recv[q]
        g = jnp.dot(x, gate[...], preferred_element_type=f32)
        u = jnp.dot(x, up[...], preferred_element_type=f32)
        return (g / (1.0 + jnp.exp(-g)) * u).astype(bf16)

    hid[me_ep, me_tp] = hidden_of(me_ep)

    up_rim.wait_recv()
    down_rim.wait_recv()
    low = rim_recv[0].astype(f32)
    high = rim_recv[1].astype(f32)
    ext[0:RIM, :] = jnp.where(me_ep > 0, low, 0.0)
    ext[RIM + rows : 2 * RIM + rows, :] = jnp.where(me_ep < ep - 1, high, 0.0)

    group_width = chan * tp // len(pool_windows)
    channel = me_tp * chan + lax.broadcasted_iota(jnp.int32, (1, chan), 1)
    seq_len = rows * ep
    for i in range(rows // chunk):
        first = RIM + i * chunk
        position = me_ep * rows + i * chunk + lax.broadcasted_iota(jnp.int32, (chunk, 1), 0)
        running = jnp.zeros((chunk, chan), f32)
        result = jnp.zeros((chunk, chan), f32)
        last = 0
        for g, window in enumerate(pool_windows):
            half = window // 2
            for o in list(range(-half, -last)) + list(range(last, half)):
                running = running + ext[first + o : first + o + chunk, :]
            last = half
            lower = jnp.maximum(position - half, 0)
            upper = jnp.minimum(position + half, seq_len)
            counts = (upper - lower).astype(f32)
            member = (channel >= g * group_width) & (channel < (g + 1) * group_width)
            result = jnp.where(member, running / counts, result)
        values = ext[first : first + chunk, :]
        pooled[me_tp, i * chunk : (i + 1) * chunk, :] = (
            (result - values) * scale[...]
        ).astype(bf16)
    for d in range(1, tp):
        tp_copy(pooled.at[me_tp], pooled.at[me_tp], po_s.at[d - 1], po_r.at[d - 1], d).start()

    def send_hidden(q, k):
        for d in range(1, tp):
            tp_copy(
                hid.at[q, me_tp], hid.at[q, me_tp], hi_s.at[k, d - 1], hi_r.at[k, d - 1], d
            ).start()

    send_hidden(me_ep, 0)

    def expert(k, carry):
        q = ep_from(k)
        ep_copy(disp_send.at[q], disp_recv.at[q], dp_s.at[k], dp_r.at[k], k).wait_recv()
        hid[q, me_tp] = hidden_of(q)
        send_hidden(q, k)
        return carry

    lax.fori_loop(1, ep, expert, 0)

    loads[3].wait()
    for d in range(1, tp):
        tp_copy(
            pooled.at[me_tp], pooled.at[tp_from(d)], po_s.at[d - 1], po_r.at[d - 1], d
        ).wait_recv()

    def mix_out(i, carry):
        at = pl.ds(pl.multiple_of(i * chunk, chunk), chunk)
        total = jnp.zeros((chunk, chan), f32)
        for p in range(tp):
            total = total + jnp.dot(
                pooled[p, at, :],
                w_mix[p * chan : (p + 1) * chan, :],
                preferred_element_type=f32,
            )
        out_m[at, :] = total.astype(bf16)
        return carry

    lax.fori_loop(0, rows // chunk, mix_out, 0)
    loads[4].wait()
    units = hid.shape[3]

    def value_of(q, k):
        for d in range(1, tp):
            tp_copy(
                hid.at[q, me_tp], hid.at[q, tp_from(d)], hi_s.at[k, d - 1], hi_r.at[k, d - 1], d
            ).wait_recv()
        total = jnp.zeros((cap, out_e.shape[1]), f32)
        for p in range(tp):
            total = total + jnp.dot(
                hid[q, p],
                down[p * units : (p + 1) * units, :],
                preferred_element_type=f32,
            )
        return total.astype(bf16)

    back_recv[me_ep] = value_of(me_ep, 0)

    def send_value(k, carry):
        q = ep_from(k)
        back_send[q] = value_of(q, k)
        ep_copy(
            back_send.at[q], back_recv.at[me_ep], bk_s.at[k], bk_r.at[k], ep - k
        ).start()
        return carry

    lax.fori_loop(1, ep, send_value, 0)

    def combine(e):
        slot = lax.broadcasted_iota(jnp.int32, (rows, cap), 1) + e * cap
        weight = jnp.where(slot == tcol[:, 0:1], rw[:, 0:1], 0.0) + jnp.where(
            slot == tcol[:, 1:2], rw[:, 1:2], 0.0
        )
        coarse = weight.astype(bf16)
        fine = (weight - coarse.astype(f32)).astype(bf16)
        v = back_recv[e]
        return jnp.dot(coarse, v, preferred_element_type=f32) + jnp.dot(
            fine, v, preferred_element_type=f32
        )

    acc[...] = combine(me_ep)

    def gather_value(k, carry):
        e = lax.rem(me_ep + k, ep)
        ep_copy(back_send.at[e], back_recv.at[e], bk_s.at[k], bk_r.at[k], k).wait_recv()
        acc[...] += combine(e)
        return carry

    lax.fori_loop(1, ep, gather_value, 0)
    out_e[...] = acc[...].astype(bf16)

    for d in range(1, tp):
        tp_copy(xe_in, xe.at[me_tp], xe_s.at[d - 1], xe_r.at[d - 1], d).wait_send()
        tp_copy(xm_in, xm.at[me_tp], xm_s.at[d - 1], xm_r.at[d - 1], d).wait_send()
        tp_copy(
            pooled.at[me_tp], pooled.at[me_tp], po_s.at[d - 1], po_r.at[d - 1], d
        ).wait_send()
    up_rim.wait_send()
    down_rim.wait_send()

    def drain(k, carry):
        e = lax.rem(me_ep + k, ep)
        q = ep_from(k)
        ep_copy(disp_send.at[e], disp_recv.at[me_ep], dp_s.at[k], dp_r.at[k], k).wait_send()
        ep_copy(back_send.at[q], back_recv.at[me_ep], bk_s.at[k], bk_r.at[k], ep - k).wait_send()
        return carry

    lax.fori_loop(1, ep, drain, 0)

    def drain_hidden(k, carry):
        q = ep_from(k)
        for d in range(1, tp):
            tp_copy(
                hid.at[q, me_tp], hid.at[q, me_tp], hi_s.at[k, d - 1], hi_r.at[k, d - 1], d
            ).wait_send()
        return carry

    lax.fori_loop(0, ep, drain_hidden, 0)


def on_device(
    mixer_rows,
    expert_rows,
    mixer_gain,
    pool_scale,
    w_in,
    w_mix_out,
    expert_gain,
    expert_gate,
    expert_up,
    expert_down,
    routes,
    route_weight,
    *,
    ep,
    tp,
):
    rows, feat = mixer_rows.shape
    width = feat * tp
    cap = (3 * TOP * rows + 2 * ep - 1) // (2 * ep)
    chan = w_in.shape[1]
    units = expert_gate.shape[2]
    flat_route = routes.reshape(-1)
    onehot = (flat_route[:, None] == jnp.arange(ep, dtype=jnp.int32)[None, :]).astype(jnp.int32)
    ranking = jnp.sum(onehot * (jnp.cumsum(onehot, axis=0) - 1), axis=1)
    target = (flat_route * cap + ranking).reshape(rows, TOP)

    vmem = pl.BlockSpec(memory_space=pltpu.VMEM)
    hbm = pl.BlockSpec(memory_space=pl.ANY)
    dma = pltpu.SemaphoreType.DMA
    return pl.pallas_call(
        functools.partial(fused, ep, tp),
        out_shape=(
            jax.ShapeDtypeStruct((rows, w_mix_out.shape[1]), bf16),
            jax.ShapeDtypeStruct((rows, expert_down.shape[2]), bf16),
        ),
        in_specs=[vmem] * 8 + [hbm] * 5,
        out_specs=(vmem, vmem),
        scratch_shapes=[
            pltpu.VMEM(w_in.shape, bf16),
            pltpu.VMEM(w_mix_out.shape, bf16),
            pltpu.VMEM(expert_gate.shape[1:], bf16),
            pltpu.VMEM(expert_up.shape[1:], bf16),
            pltpu.VMEM(expert_down.shape[1:], bf16),
            pltpu.VMEM((tp, rows, feat), bf16),
            pltpu.VMEM((tp, rows, feat), bf16),
            pltpu.VMEM((rows, width), bf16),
            pltpu.VMEM((ep, cap, width), bf16),
            pltpu.VMEM((ep, cap, width), bf16),
            pltpu.VMEM((ep, tp, cap, units), bf16),
            pltpu.VMEM((tp, rows, chan), bf16),
            pltpu.VMEM((ep, cap, expert_down.shape[2]), bf16),
            pltpu.VMEM((ep, cap, expert_down.shape[2]), bf16),
            pltpu.VMEM((rows + 2 * RIM, chan), f32),
            pltpu.VMEM((2, RIM, chan), bf16),
            pltpu.VMEM((2, RIM, chan), bf16),
            pltpu.VMEM((rows, expert_down.shape[2]), f32),
            dma((5,)),
            dma((tp - 1,)),
            dma((tp - 1,)),
            dma((tp - 1,)),
            dma((tp - 1,)),
            dma((ep,)),
            dma((ep,)),
            dma((2,)),
            dma((2,)),
            dma((tp - 1,)),
            dma((tp - 1,)),
            dma((ep, tp - 1)),
            dma((ep, tp - 1)),
            dma((ep,)),
            dma((ep,)),
        ],
        compiler_params=pltpu.CompilerParams(
            collective_id=0, has_side_effects=True, vmem_limit_bytes=62 * 1024 * 1024
        ),
    )(
        mixer_rows,
        expert_rows,
        mixer_gain.reshape(1, width),
        expert_gain.reshape(1, width),
        pool_scale.reshape(1, chan),
        target.T,
        target,
        route_weight,
        w_in,
        w_mix_out,
        expert_gate.reshape(expert_gate.shape[1:]),
        expert_up.reshape(expert_up.shape[1:]),
        expert_down.reshape(expert_down.shape[1:]),
    )


def solution(mesh):
    return jax.shard_map(
        functools.partial(on_device, ep=mesh.shape["ep"], tp=mesh.shape["tp"]),
        mesh=mesh,
        in_specs=(
            P("ep", "tp"),
            P("ep", "tp"),
            P(),
            P("tp"),
            P(None, "tp"),
            P(None, "tp"),
            P(),
            P("ep", None, "tp"),
            P("ep", None, "tp"),
            P("ep", None, "tp"),
            P("ep", None),
            P("ep", None),
        ),
        out_specs=(P("ep", "tp"), P("ep", "tp")),
        check_vma=False,
    )
```

```python
import functools

import jax
import jax.numpy as jnp
from jax import lax
from jax.experimental import pallas as pl
from jax.experimental.pallas import tpu as pltpu
from jax.sharding import PartitionSpec as P

TOP = 2
norm_eps = 1e-05
pool_windows = (2, 4, 8, 16)
RIM = 16
MESH = pl.DeviceIdType.MESH
f32 = jnp.float32
bf16 = jnp.bfloat16


def fused(
    ep,
    tp,
    xm_in,
    xe_in,
    gain_m,
    gain_e,
    scale,
    trow,
    tcol,
    rw,
    w_in_h,
    w_mix_h,
    gate_h,
    up_h,
    down_h,
    out_m,
    out_e,
    w_in,
    w_mix,
    gate,
    up,
    down,
    xm,
    normed,
    block,
    disp_send,
    slots,
    hid,
    pooled,
    back_send,
    back_recv,
    ext,
    rim_send,
    rim_recv,
    acc,
    w_sem,
    sl_s,
    sl_r,
    xm_s,
    xm_r,
    dp_s,
    dp_r,
    rim_s,
    rim_r,
    po_s,
    po_r,
    hi_s,
    hi_r,
    bk_s,
    bk_r,
):
    me_ep = lax.axis_index("ep")
    me_tp = lax.axis_index("tp")
    rows, feat = xm_in.shape
    cap = slots.shape[2]
    chan = out_m.shape[1]
    width = feat * tp
    chunk = min(rows, 128)

    barrier = pltpu.get_barrier_semaphore()
    for d in range(1, tp):
        pl.semaphore_signal(
            barrier, inc=1, device_id={"tp": lax.rem(me_tp + d, tp)}, device_id_type=MESH
        )
    for d in range(1, ep):
        pl.semaphore_signal(
            barrier, inc=1, device_id={"ep": lax.rem(me_ep + d, ep)}, device_id_type=MESH
        )
    pl.semaphore_wait(barrier, tp + ep - 2)

    def tp_copy(ref, s, r, peer):
        return pltpu.make_async_remote_copy(
            src_ref=ref,
            dst_ref=ref,
            send_sem=s,
            recv_sem=r,
            device_id={"tp": peer},
            device_id_type=MESH,
        )

    def ep_copy(src, dst, s, r, d):
        return pltpu.make_async_remote_copy(
            src_ref=src,
            dst_ref=dst,
            send_sem=s,
            recv_sem=r,
            device_id={"ep": lax.rem(me_ep + d, ep)},
            device_id_type=MESH,
        )

    relayed = tp == 4
    col = lax.rem(me_tp, 2)
    row = me_tp // 2
    beside = row * 2 + (1 - col)
    above = (1 - row) * 2 + col
    across = (1 - row) * 2 + (1 - col)

    def send(slot, s, r):
        if relayed:
            tp_copy(slot(me_tp), s(0), r(0), beside).start()
            tp_copy(slot(me_tp), s(1), r(1), above).start()
        else:
            for d in range(1, tp):
                tp_copy(slot(me_tp), s(d - 1), r(d - 1), lax.rem(me_tp + d, tp)).start()

    def relay(slot, s, r, turn):
        if relayed:
            tp_copy(slot(beside), s(0), r(0), beside).wait_recv()
            tp_copy(slot(above), s(1), r(1), above).wait_recv()
            source = (1 - turn) * beside + turn * above
            peer = (1 - turn) * above + turn * beside
            tp_copy(slot(source), s(2), r(2), peer).start()

    def finish(slot, s, r):
        if relayed:
            tp_copy(slot(across), s(2), r(2), across).wait_recv()
        else:
            for d in range(1, tp):
                p = lax.rem(me_tp - d + tp, tp)
                tp_copy(slot(p), s(d - 1), r(d - 1), p).wait_recv()

    def drain(slot, s, r):
        for d in range(1, tp):
            tp_copy(slot(me_tp), s(d - 1), r(d - 1), lax.rem(me_tp + d, tp)).wait_send()

    def mixer_part():
        return lambda p: xm.at[p], lambda j: xm_s.at[j], lambda j: xm_r.at[j]

    def pooled_part():
        return lambda p: pooled.at[p], lambda j: po_s.at[j], lambda j: po_r.at[j]

    def slot_part(k):
        q = ep_from(k)
        return lambda p: slots.at[q, p], lambda j: sl_s.at[k, j], lambda j: sl_r.at[k, j]

    def hidden_part(k):
        q = ep_from(k)
        return lambda p: hid.at[q, p], lambda j: hi_s.at[k, j], lambda j: hi_r.at[k, j]

    def ep_from(d):
        return lax.rem(me_ep - d + ep, ep)

    xm_load = pltpu.make_async_copy(xm_in, xm.at[me_tp], w_sem.at[5])
    xm_load.start()
    xm_load.wait()
    send(*mixer_part())

    loads = [
        pltpu.make_async_copy(h, v, w_sem.at[i])
        for i, (h, v) in enumerate(
            ((w_in_h, w_in), (gate_h, gate), (up_h, up), (w_mix_h, w_mix), (down_h, down))
        )
    ]
    for load in loads:
        load.start()

    def picked_rows(e):
        slot = lax.broadcasted_iota(jnp.int32, (cap, rows), 0) + e * cap
        hit = (slot == trow[0:1, :]) | (slot == trow[1:2, :])
        pick = jnp.where(hit, 1.0, 0.0).astype(bf16)
        return jnp.dot(pick, xe_in[...], preferred_element_type=f32).astype(bf16)

    def send_rows(d, carry):
        e = lax.rem(me_ep + d, ep)
        disp_send[e] = picked_rows(e)
        ep_copy(disp_send.at[e], slots.at[me_ep, me_tp], dp_s.at[d], dp_r.at[d], d).start()
        return carry

    lax.fori_loop(1, ep, send_rows, 0)
    slots[me_ep, me_tp] = picked_rows(me_ep)
    send(*slot_part(0))
    relay(*mixer_part(), 0)

    def pass_slots(k, carry):
        q = ep_from(k)
        ep_copy(disp_send.at[q], slots.at[q, me_tp], dp_s.at[k], dp_r.at[k], k).wait_recv()
        send(*slot_part(k))
        relay(*slot_part(k - 1), lax.rem(k, 2))
        return carry

    early = ep // 2
    lax.fori_loop(1, early, pass_slots, 0)

    def norm_rows(parts, gain):
        parts = [v.astype(f32) for v in parts]
        mean = sum(jnp.sum(v, axis=-1, keepdims=True) for v in parts) / width
        parts = [v - mean for v in parts]
        spread = sum(jnp.sum(v * v, axis=-1, keepdims=True) for v in parts) / width
        inv = lax.rsqrt(spread + norm_eps)
        return [
            (v * inv * gain[:, p * feat : (p + 1) * feat]).astype(bf16)
            for p, v in enumerate(parts)
        ]

    finish(*mixer_part())
    loads[0].wait()

    def project(i, carry):
        at = pl.ds(pl.multiple_of(i * chunk, chunk), chunk)
        for p, v in enumerate(norm_rows([xm[p, at, :] for p in range(tp)], gain_m)):
            normed[:, p * feat : (p + 1) * feat] = v
        inner = jnp.dot(normed[...], w_in[...], preferred_element_type=f32).astype(bf16)
        ext[pl.ds(pl.multiple_of(RIM + i * chunk, RIM), chunk), :] = inner.astype(f32)
        return carry

    lax.fori_loop(0, rows // chunk, project, 0)
    rim_send[0] = ext[rows : rows + RIM, :].astype(bf16)
    rim_send[1] = ext[RIM : 2 * RIM, :].astype(bf16)
    up_rim = ep_copy(rim_send.at[0], rim_recv.at[0], rim_s.at[0], rim_r.at[0], 1)
    down_rim = ep_copy(rim_send.at[1], rim_recv.at[1], rim_s.at[1], rim_r.at[1], ep - 1)
    up_rim.start()
    down_rim.start()

    lax.fori_loop(early, ep, pass_slots, 0)
    relay(*slot_part(ep - 1), ep % 2)

    up_rim.wait_recv()
    down_rim.wait_recv()
    low = rim_recv[0].astype(f32)
    high = rim_recv[1].astype(f32)
    ext[0:RIM, :] = jnp.where(me_ep > 0, low, 0.0)
    ext[RIM + rows : 2 * RIM + rows, :] = jnp.where(me_ep < ep - 1, high, 0.0)

    group_width = chan * tp // len(pool_windows)
    channel = me_tp * chan + lax.broadcasted_iota(jnp.int32, (1, chan), 1)
    seq_len = rows * ep
    for i in range(rows // chunk):
        first = RIM + i * chunk
        position = me_ep * rows + i * chunk + lax.broadcasted_iota(jnp.int32, (chunk, 1), 0)
        running = jnp.zeros((chunk, chan), f32)
        result = jnp.zeros((chunk, chan), f32)
        last = 0
        for g, window in enumerate(pool_windows):
            half = window // 2
            for o in list(range(-half, -last)) + list(range(last, half)):
                running = running + ext[first + o : first + o + chunk, :]
            last = half
            lower = jnp.maximum(position - half, 0)
            upper = jnp.minimum(position + half, seq_len)
            counts = (upper - lower).astype(f32)
            member = (channel >= g * group_width) & (channel < (g + 1) * group_width)
            result = jnp.where(member, running / counts, result)
        values = ext[first : first + chunk, :]
        pooled[me_tp, i * chunk : (i + 1) * chunk, :] = (
            (result - values) * scale[...]
        ).astype(bf16)
    send(*pooled_part())

    loads[1].wait()
    loads[2].wait()

    def hidden_step(k):
        q = ep_from(k)
        finish(*slot_part(k))
        for p, v in enumerate(norm_rows([slots[q, p] for p in range(tp)], gain_e)):
            block[:, p * feat : (p + 1) * feat] = v
        x = block[...]
        g = jnp.dot(x, gate[...], preferred_element_type=f32)
        u = jnp.dot(x, up[...], preferred_element_type=f32)
        hid[q, me_tp] = (g / (1.0 + jnp.exp(-g)) * u).astype(bf16)
        send(*hidden_part(k))

    units = hid.shape[3]

    def value_step(k):
        q = ep_from(k)
        finish(*hidden_part(k))
        total = jnp.zeros((cap, out_e.shape[1]), f32)
        for p in range(tp):
            total = total + jnp.dot(
                hid[q, p],
                down[p * units : (p + 1) * units, :],
                preferred_element_type=f32,
            )
        return total.astype(bf16)

    def send_value(k):
        q = ep_from(k)
        back_send[q] = value_step(k)
        ep_copy(back_send.at[q], back_recv.at[me_ep], bk_s.at[k], bk_r.at[k], ep - k).start()

    hidden_step(0)
    relay(*pooled_part(), 1)
    hidden_step(1)
    relay(*hidden_part(0), 1)

    loads[3].wait()
    finish(*pooled_part())

    def mix_out(i, carry):
        at = pl.ds(pl.multiple_of(i * chunk, chunk), chunk)
        total = jnp.zeros((chunk, chan), f32)
        for p in range(tp):
            total = total + jnp.dot(
                pooled[p, at, :],
                w_mix[p * chan : (p + 1) * chan, :],
                preferred_element_type=f32,
            )
        out_m[at, :] = total.astype(bf16)
        return carry

    lax.fori_loop(0, rows // chunk, mix_out, 0)
    loads[4].wait()

    hidden_step(2)
    relay(*hidden_part(1), 0)
    back_recv[me_ep] = value_step(0)

    def expert(k, carry):
        hidden_step(k)
        relay(*hidden_part(k - 1), lax.rem(k, 2))
        send_value(k - 2)
        return carry

    lax.fori_loop(3, ep, expert, 0)
    relay(*hidden_part(ep - 1), ep % 2)
    send_value(ep - 2)
    send_value(ep - 1)

    def combine(e):
        slot = lax.broadcasted_iota(jnp.int32, (rows, cap), 1) + e * cap
        weight = jnp.where(slot == tcol[:, 0:1], rw[:, 0:1], 0.0) + jnp.where(
            slot == tcol[:, 1:2], rw[:, 1:2], 0.0
        )
        coarse = weight.astype(bf16)
        fine = (weight - coarse.astype(f32)).astype(bf16)
        v = back_recv[e]
        return jnp.dot(coarse, v, preferred_element_type=f32) + jnp.dot(
            fine, v, preferred_element_type=f32
        )

    acc[...] = combine(me_ep)

    def gather_value(k, carry):
        e = lax.rem(me_ep + k, ep)
        ep_copy(back_send.at[e], back_recv.at[e], bk_s.at[k], bk_r.at[k], k).wait_recv()
        acc[...] += combine(e)
        return carry

    lax.fori_loop(1, ep, gather_value, 0)
    out_e[...] = acc[...].astype(bf16)

    drain(*mixer_part())
    drain(*pooled_part())
    up_rim.wait_send()
    down_rim.wait_send()

    def drain_ep(k, carry):
        e = lax.rem(me_ep + k, ep)
        q = ep_from(k)
        ep_copy(disp_send.at[e], slots.at[me_ep, me_tp], dp_s.at[k], dp_r.at[k], k).wait_send()
        ep_copy(back_send.at[q], back_recv.at[me_ep], bk_s.at[k], bk_r.at[k], ep - k).wait_send()
        return carry

    lax.fori_loop(1, ep, drain_ep, 0)

    def drain_tp(k, carry):
        drain(*slot_part(k))
        drain(*hidden_part(k))
        return carry

    lax.fori_loop(0, ep, drain_tp, 0)


def on_device(
    mixer_rows,
    expert_rows,
    mixer_gain,
    pool_scale,
    w_in,
    w_mix_out,
    expert_gain,
    expert_gate,
    expert_up,
    expert_down,
    routes,
    route_weight,
    *,
    ep,
    tp,
):
    rows, feat = mixer_rows.shape
    width = feat * tp
    cap = (3 * TOP * rows + 2 * ep - 1) // (2 * ep)
    chan = w_in.shape[1]
    units = expert_gate.shape[2]
    flat_route = routes.reshape(-1)
    onehot = (flat_route[:, None] == jnp.arange(ep, dtype=jnp.int32)[None, :]).astype(jnp.int32)
    ranking = jnp.sum(onehot * (jnp.cumsum(onehot, axis=0) - 1), axis=1)
    target = (flat_route * cap + ranking).reshape(rows, TOP)

    vmem = pl.BlockSpec(memory_space=pltpu.VMEM)
    hbm = pl.BlockSpec(memory_space=pl.ANY)
    dma = pltpu.SemaphoreType.DMA
    return pl.pallas_call(
        functools.partial(fused, ep, tp),
        out_shape=(
            jax.ShapeDtypeStruct((rows, w_mix_out.shape[1]), bf16),
            jax.ShapeDtypeStruct((rows, expert_down.shape[2]), bf16),
        ),
        in_specs=[vmem] * 8 + [hbm] * 5,
        out_specs=(vmem, vmem),
        scratch_shapes=[
            pltpu.VMEM(w_in.shape, bf16),
            pltpu.VMEM(w_mix_out.shape, bf16),
            pltpu.VMEM(expert_gate.shape[1:], bf16),
            pltpu.VMEM(expert_up.shape[1:], bf16),
            pltpu.VMEM(expert_down.shape[1:], bf16),
            pltpu.VMEM((tp, rows, feat), bf16),
            pltpu.VMEM((min(rows, 128), width), bf16),
            pltpu.VMEM((cap, width), bf16),
            pltpu.VMEM((ep, cap, feat), bf16),
            pltpu.VMEM((ep, tp, cap, feat), bf16),
            pltpu.VMEM((ep, tp, cap, units), bf16),
            pltpu.VMEM((tp, rows, chan), bf16),
            pltpu.VMEM((ep, cap, expert_down.shape[2]), bf16),
            pltpu.VMEM((ep, cap, expert_down.shape[2]), bf16),
            pltpu.VMEM((rows + 2 * RIM, chan), f32),
            pltpu.VMEM((2, RIM, chan), bf16),
            pltpu.VMEM((2, RIM, chan), bf16),
            pltpu.VMEM((rows, expert_down.shape[2]), f32),
            dma((6,)),
            dma((ep, tp - 1)),
            dma((ep, tp - 1)),
            dma((tp - 1,)),
            dma((tp - 1,)),
            dma((ep,)),
            dma((ep,)),
            dma((2,)),
            dma((2,)),
            dma((tp - 1,)),
            dma((tp - 1,)),
            dma((ep, tp - 1)),
            dma((ep, tp - 1)),
            dma((ep,)),
            dma((ep,)),
        ],
        compiler_params=pltpu.CompilerParams(
            collective_id=0, has_side_effects=True, vmem_limit_bytes=62 * 1024 * 1024
        ),
    )(
        mixer_rows,
        expert_rows,
        mixer_gain.reshape(1, width),
        expert_gain.reshape(1, width),
        pool_scale.reshape(1, chan),
        target.T,
        target,
        route_weight,
        w_in,
        w_mix_out,
        expert_gate.reshape(expert_gate.shape[1:]),
        expert_up.reshape(expert_up.shape[1:]),
        expert_down.reshape(expert_down.shape[1:]),
    )


def solution(mesh):
    return jax.shard_map(
        functools.partial(on_device, ep=mesh.shape["ep"], tp=mesh.shape["tp"]),
        mesh=mesh,
        in_specs=(
            P("ep", "tp"),
            P("ep", "tp"),
            P(),
            P("tp"),
            P(None, "tp"),
            P(None, "tp"),
            P(),
            P("ep", None, "tp"),
            P("ep", None, "tp"),
            P("ep", None, "tp"),
            P("ep", None),
            P("ep", None),
        ),
        out_specs=(P("ep", "tp"), P("ep", "tp")),
        check_vma=False,
    )
```

```python
import functools

import jax
import jax.numpy as jnp
from jax import lax
from jax.experimental import pallas as pl
from jax.experimental.pallas import tpu as pltpu
from jax.sharding import PartitionSpec as P

TOP = 2
norm_eps = 1e-05
pool_windows = (2, 4, 8, 16)
RIM = 16
MESH = pl.DeviceIdType.MESH
f32 = jnp.float32
bf16 = jnp.bfloat16


def fused(
    ep,
    tp,
    xm_in,
    xe_in,
    gain_m,
    gain_e,
    scale,
    route_rows,
    route_cols,
    rw,
    w_in_h,
    w_mix_h,
    gate_h,
    up_h,
    down_h,
    out_m,
    out_e,
    w_in,
    w_mix,
    gate,
    up,
    down,
    xm,
    normed,
    block,
    disp_send,
    slots,
    hid,
    pooled,
    back_send,
    back_recv,
    ext,
    rim_send,
    rim_recv,
    acc,
    tcol,
    w_sem,
    sl_s,
    sl_r,
    xm_s,
    xm_r,
    dp_s,
    dp_r,
    rim_s,
    rim_r,
    po_s,
    po_r,
    hi_s,
    hi_r,
    bk_s,
    bk_r,
):
    me_ep = lax.axis_index("ep")
    me_tp = lax.axis_index("tp")
    rows, feat = xm_in.shape
    cap = slots.shape[2]
    chan = out_m.shape[1]
    width = feat * tp
    chunk = min(rows, 128)

    barrier = pltpu.get_barrier_semaphore()
    for d in range(1, tp):
        pl.semaphore_signal(
            barrier, inc=1, device_id={"tp": lax.rem(me_tp + d, tp)}, device_id_type=MESH
        )
    for d in range(1, ep):
        pl.semaphore_signal(
            barrier, inc=1, device_id={"ep": lax.rem(me_ep + d, ep)}, device_id_type=MESH
        )
    pl.semaphore_wait(barrier, tp + ep - 2)

    def tp_copy(ref, s, r, peer):
        return pltpu.make_async_remote_copy(
            src_ref=ref,
            dst_ref=ref,
            send_sem=s,
            recv_sem=r,
            device_id={"tp": peer},
            device_id_type=MESH,
        )

    def ep_copy(src, dst, s, r, d):
        return pltpu.make_async_remote_copy(
            src_ref=src,
            dst_ref=dst,
            send_sem=s,
            recv_sem=r,
            device_id={"ep": lax.rem(me_ep + d, ep)},
            device_id_type=MESH,
        )

    relayed = tp == 4
    col = lax.rem(me_tp, 2)
    row = me_tp // 2
    beside = row * 2 + (1 - col)
    above = (1 - row) * 2 + col
    across = (1 - row) * 2 + (1 - col)

    def send(slot, s, r):
        if relayed:
            tp_copy(slot(me_tp), s(0), r(0), beside).start()
            tp_copy(slot(me_tp), s(1), r(1), above).start()
        else:
            for d in range(1, tp):
                tp_copy(slot(me_tp), s(d - 1), r(d - 1), lax.rem(me_tp + d, tp)).start()

    def relay(slot, s, r, turn):
        if relayed:
            tp_copy(slot(beside), s(0), r(0), beside).wait_recv()
            tp_copy(slot(above), s(1), r(1), above).wait_recv()
            source = (1 - turn) * beside + turn * above
            peer = (1 - turn) * above + turn * beside
            tp_copy(slot(source), s(2), r(2), peer).start()

    def finish(slot, s, r):
        if relayed:
            tp_copy(slot(across), s(2), r(2), across).wait_recv()
        else:
            for d in range(1, tp):
                p = lax.rem(me_tp - d + tp, tp)
                tp_copy(slot(p), s(d - 1), r(d - 1), p).wait_recv()

    def drain(slot, s, r):
        for d in range(1, tp):
            tp_copy(slot(me_tp), s(d - 1), r(d - 1), lax.rem(me_tp + d, tp)).wait_send()

    def mixer_part():
        return lambda p: xm.at[p], lambda j: xm_s.at[j], lambda j: xm_r.at[j]

    def pooled_part():
        return lambda p: pooled.at[p], lambda j: po_s.at[j], lambda j: po_r.at[j]

    def slot_part(k):
        q = ep_from(k)
        return lambda p: slots.at[q, p], lambda j: sl_s.at[k, j], lambda j: sl_r.at[k, j]

    def hidden_part(k):
        q = ep_from(k)
        return lambda p: hid.at[q, p], lambda j: hi_s.at[k, j], lambda j: hi_r.at[k, j]

    def ep_from(d):
        return lax.rem(me_ep - d + ep, ep)

    xm_load = pltpu.make_async_copy(xm_in, xm.at[me_tp], w_sem.at[5])
    xm_load.start()
    xm_load.wait()
    send(*mixer_part())

    loads = [
        pltpu.make_async_copy(h, v, w_sem.at[i])
        for i, (h, v) in enumerate(
            ((w_in_h, w_in), (gate_h, gate), (up_h, up), (w_mix_h, w_mix), (down_h, down))
        )
    ]
    for load in loads:
        load.start()

    t0 = lax.broadcasted_iota(jnp.int32, (rows, rows), 0)
    t1 = lax.broadcasted_iota(jnp.int32, (rows, rows), 1)
    names = lax.broadcasted_iota(jnp.int32, (ep, rows), 0)
    named = [jnp.where(route_rows[j : j + 1, :] == names, 1.0, 0.0) for j in range(TOP)]
    ahead = jnp.dot(
        sum(named).astype(bf16),
        jnp.where(t0 < t1, 1.0, 0.0).astype(bf16),
        preferred_element_type=f32,
    )
    trow = [
        route_rows[j : j + 1, :] * cap
        + jnp.sum(named[j] * ahead, axis=0, keepdims=True).astype(jnp.int32)
        for j in range(TOP)
    ]
    names = lax.broadcasted_iota(jnp.int32, (rows, ep), 1)
    named = [jnp.where(route_cols[:, j : j + 1] == names, 1.0, 0.0) for j in range(TOP)]
    ahead = jnp.dot(
        jnp.where(t1 < t0, 1.0, 0.0).astype(bf16),
        sum(named).astype(bf16),
        preferred_element_type=f32,
    )
    for j in range(TOP):
        tcol[:, j : j + 1] = route_cols[:, j : j + 1] * cap + jnp.sum(
            named[j] * ahead, axis=1, keepdims=True
        ).astype(jnp.int32)

    def picked_rows(e):
        slot = lax.broadcasted_iota(jnp.int32, (cap, rows), 0) + e * cap
        hit = (slot == trow[0]) | (slot == trow[1])
        pick = jnp.where(hit, 1.0, 0.0).astype(bf16)
        return jnp.dot(pick, xe_in[...], preferred_element_type=f32).astype(bf16)

    def send_rows(d, carry):
        e = lax.rem(me_ep + d, ep)
        disp_send[e] = picked_rows(e)
        ep_copy(disp_send.at[e], slots.at[me_ep, me_tp], dp_s.at[d], dp_r.at[d], d).start()
        return carry

    lax.fori_loop(1, ep, send_rows, 0)
    slots[me_ep, me_tp] = picked_rows(me_ep)
    relay(*mixer_part(), 0)

    def arrive(k):
        q = ep_from(k)
        ep_copy(disp_send.at[q], slots.at[q, me_tp], dp_s.at[k], dp_r.at[k], k).wait_recv()
        send(*slot_part(k))

    arrive(1)

    def pass_slots(k, carry):
        arrive(k)
        relay(*slot_part(k - 1), lax.rem(k, 2))
        return carry

    early = ep // 2
    lax.fori_loop(2, early, pass_slots, 0)

    def norm_rows(parts, gain):
        parts = [v.astype(f32) for v in parts]
        mean = sum(jnp.sum(v, axis=-1, keepdims=True) for v in parts) / width
        parts = [v - mean for v in parts]
        spread = sum(jnp.sum(v * v, axis=-1, keepdims=True) for v in parts) / width
        inv = lax.rsqrt(spread + norm_eps)
        return [
            (v * inv * gain[:, p * feat : (p + 1) * feat]).astype(bf16)
            for p, v in enumerate(parts)
        ]

    finish(*mixer_part())
    loads[0].wait()

    def project(i, carry):
        at = pl.ds(pl.multiple_of(i * chunk, chunk), chunk)
        for p, v in enumerate(norm_rows([xm[p, at, :] for p in range(tp)], gain_m)):
            normed[:, p * feat : (p + 1) * feat] = v
        inner = jnp.dot(normed[...], w_in[...], preferred_element_type=f32).astype(bf16)
        ext[pl.ds(pl.multiple_of(RIM + i * chunk, RIM), chunk), :] = inner.astype(f32)
        return carry

    lax.fori_loop(0, rows // chunk, project, 0)
    rim_send[0] = ext[rows : rows + RIM, :].astype(bf16)
    rim_send[1] = ext[RIM : 2 * RIM, :].astype(bf16)
    up_rim = ep_copy(rim_send.at[0], rim_recv.at[0], rim_s.at[0], rim_r.at[0], 1)
    down_rim = ep_copy(rim_send.at[1], rim_recv.at[1], rim_s.at[1], rim_r.at[1], ep - 1)
    up_rim.start()
    down_rim.start()

    lax.fori_loop(early, ep - 1, pass_slots, 0)

    up_rim.wait_recv()
    down_rim.wait_recv()
    low = rim_recv[0].astype(f32)
    high = rim_recv[1].astype(f32)
    ext[0:RIM, :] = jnp.where(me_ep > 0, low, 0.0)
    ext[RIM + rows : 2 * RIM + rows, :] = jnp.where(me_ep < ep - 1, high, 0.0)

    group_width = chan * tp // len(pool_windows)
    channel = me_tp * chan + lax.broadcasted_iota(jnp.int32, (1, chan), 1)
    seq_len = rows * ep
    for i in range(rows // chunk):
        first = RIM + i * chunk
        position = me_ep * rows + i * chunk + lax.broadcasted_iota(jnp.int32, (chunk, 1), 0)
        running = jnp.zeros((chunk, chan), f32)
        result = jnp.zeros((chunk, chan), f32)
        last = 0
        for g, window in enumerate(pool_windows):
            half = window // 2
            for o in list(range(-half, -last)) + list(range(last, half)):
                running = running + ext[first + o : first + o + chunk, :]
            last = half
            lower = jnp.maximum(position - half, 0)
            upper = jnp.minimum(position + half, seq_len)
            counts = (upper - lower).astype(f32)
            member = (channel >= g * group_width) & (channel < (g + 1) * group_width)
            result = jnp.where(member, running / counts, result)
        values = ext[first : first + chunk, :]
        pooled[me_tp, i * chunk : (i + 1) * chunk, :] = (
            (result - values) * scale[...]
        ).astype(bf16)
    send(*pooled_part())
    pass_slots(ep - 1, 0)
    send(*slot_part(0))

    loads[1].wait()
    loads[2].wait()

    def hidden_step(k):
        q = ep_from(k)
        finish(*slot_part(k))
        for p, v in enumerate(norm_rows([slots[q, p] for p in range(tp)], gain_e)):
            block[:, p * feat : (p + 1) * feat] = v
        x = block[...]
        g = jnp.dot(x, gate[...], preferred_element_type=f32)
        u = jnp.dot(x, up[...], preferred_element_type=f32)
        hid[q, me_tp] = (g / (1.0 + jnp.exp(-g)) * u).astype(bf16)
        send(*hidden_part(k))

    units = hid.shape[3]

    def value_step(k):
        q = ep_from(k)
        finish(*hidden_part(k))
        total = jnp.zeros((cap, out_e.shape[1]), f32)
        for p in range(tp):
            total = total + jnp.dot(
                hid[q, p],
                down[p * units : (p + 1) * units, :],
                preferred_element_type=f32,
            )
        return total.astype(bf16)

    def send_value(k):
        q = ep_from(k)
        back_send[q] = value_step(k)
        ep_copy(back_send.at[q], back_recv.at[me_ep], bk_s.at[k], bk_r.at[k], ep - k).start()

    hidden_step(1)
    relay(*slot_part(ep - 1), ep % 2)
    hidden_step(2)
    relay(*slot_part(0), 1 - ep % 2)
    relay(*pooled_part(), 1)
    relay(*hidden_part(1), 0)

    loads[3].wait()
    finish(*pooled_part())

    def mix_out(i, carry):
        at = pl.ds(pl.multiple_of(i * chunk, chunk), chunk)
        total = jnp.zeros((chunk, chan), f32)
        for p in range(tp):
            total = total + jnp.dot(
                pooled[p, at, :],
                w_mix[p * chan : (p + 1) * chan, :],
                preferred_element_type=f32,
            )
        out_m[at, :] = total.astype(bf16)
        return carry

    lax.fori_loop(0, rows // chunk, mix_out, 0)
    loads[4].wait()

    def expert(k, carry):
        hidden_step(k)
        relay(*hidden_part(k - 1), lax.rem(k, 2))
        send_value(k - 2)
        return carry

    lax.fori_loop(3, ep, expert, 0)
    hidden_step(0)
    relay(*hidden_part(ep - 1), ep % 2)
    send_value(ep - 2)
    relay(*hidden_part(0), 1 - ep % 2)
    send_value(ep - 1)
    back_recv[me_ep] = value_step(0)

    def combine(e):
        slot = lax.broadcasted_iota(jnp.int32, (rows, cap), 1) + e * cap
        weight = jnp.where(slot == tcol[:, 0:1], rw[:, 0:1], 0.0) + jnp.where(
            slot == tcol[:, 1:2], rw[:, 1:2], 0.0
        )
        coarse = weight.astype(bf16)
        fine = (weight - coarse.astype(f32)).astype(bf16)
        v = back_recv[e]
        return jnp.dot(coarse, v, preferred_element_type=f32) + jnp.dot(
            fine, v, preferred_element_type=f32
        )

    acc[...] = combine(me_ep)

    def gather_value(k, carry):
        e = lax.rem(me_ep + k, ep)
        ep_copy(back_send.at[e], back_recv.at[e], bk_s.at[k], bk_r.at[k], k).wait_recv()
        acc[...] += combine(e)
        return carry

    lax.fori_loop(1, ep, gather_value, 0)
    out_e[...] = acc[...].astype(bf16)

    drain(*mixer_part())
    drain(*pooled_part())
    up_rim.wait_send()
    down_rim.wait_send()

    def drain_ep(k, carry):
        e = lax.rem(me_ep + k, ep)
        q = ep_from(k)
        ep_copy(disp_send.at[e], slots.at[me_ep, me_tp], dp_s.at[k], dp_r.at[k], k).wait_send()
        ep_copy(back_send.at[q], back_recv.at[me_ep], bk_s.at[k], bk_r.at[k], ep - k).wait_send()
        return carry

    lax.fori_loop(1, ep, drain_ep, 0)

    def drain_tp(k, carry):
        drain(*slot_part(k))
        drain(*hidden_part(k))
        return carry

    lax.fori_loop(0, ep, drain_tp, 0)


def on_device(
    mixer_rows,
    expert_rows,
    mixer_gain,
    pool_scale,
    w_in,
    w_mix_out,
    expert_gain,
    expert_gate,
    expert_up,
    expert_down,
    routes,
    route_weight,
    *,
    ep,
    tp,
):
    rows, feat = mixer_rows.shape
    width = feat * tp
    cap = (3 * TOP * rows + 2 * ep - 1) // (2 * ep)
    chan = w_in.shape[1]
    units = expert_gate.shape[2]
    vmem = pl.BlockSpec(memory_space=pltpu.VMEM)
    hbm = pl.BlockSpec(memory_space=pl.ANY)
    dma = pltpu.SemaphoreType.DMA
    return pl.pallas_call(
        functools.partial(fused, ep, tp),
        out_shape=(
            jax.ShapeDtypeStruct((rows, w_mix_out.shape[1]), bf16),
            jax.ShapeDtypeStruct((rows, expert_down.shape[2]), bf16),
        ),
        in_specs=[vmem] * 8 + [hbm] * 5,
        out_specs=(vmem, vmem),
        scratch_shapes=[
            pltpu.VMEM(w_in.shape, bf16),
            pltpu.VMEM(w_mix_out.shape, bf16),
            pltpu.VMEM(expert_gate.shape[1:], bf16),
            pltpu.VMEM(expert_up.shape[1:], bf16),
            pltpu.VMEM(expert_down.shape[1:], bf16),
            pltpu.VMEM((tp, rows, feat), bf16),
            pltpu.VMEM((min(rows, 128), width), bf16),
            pltpu.VMEM((cap, width), bf16),
            pltpu.VMEM((ep, cap, feat), bf16),
            pltpu.VMEM((ep, tp, cap, feat), bf16),
            pltpu.VMEM((ep, tp, cap, units), bf16),
            pltpu.VMEM((tp, rows, chan), bf16),
            pltpu.VMEM((ep, cap, expert_down.shape[2]), bf16),
            pltpu.VMEM((ep, cap, expert_down.shape[2]), bf16),
            pltpu.VMEM((rows + 2 * RIM, chan), f32),
            pltpu.VMEM((2, RIM, chan), bf16),
            pltpu.VMEM((2, RIM, chan), bf16),
            pltpu.VMEM((rows, expert_down.shape[2]), f32),
            pltpu.VMEM((rows, TOP), jnp.int32),
            dma((6,)),
            dma((ep, tp - 1)),
            dma((ep, tp - 1)),
            dma((tp - 1,)),
            dma((tp - 1,)),
            dma((ep,)),
            dma((ep,)),
            dma((2,)),
            dma((2,)),
            dma((tp - 1,)),
            dma((tp - 1,)),
            dma((ep, tp - 1)),
            dma((ep, tp - 1)),
            dma((ep,)),
            dma((ep,)),
        ],
        compiler_params=pltpu.CompilerParams(
            collective_id=0, has_side_effects=True, vmem_limit_bytes=62 * 1024 * 1024
        ),
    )(
        mixer_rows,
        expert_rows,
        mixer_gain.reshape(1, width),
        expert_gain.reshape(1, width),
        pool_scale.reshape(1, chan),
        routes.T,
        routes,
        route_weight,
        w_in,
        w_mix_out,
        expert_gate.reshape(expert_gate.shape[1:]),
        expert_up.reshape(expert_up.shape[1:]),
        expert_down.reshape(expert_down.shape[1:]),
    )


def solution(mesh):
    return jax.shard_map(
        functools.partial(on_device, ep=mesh.shape["ep"], tp=mesh.shape["tp"]),
        mesh=mesh,
        in_specs=(
            P("ep", "tp"),
            P("ep", "tp"),
            P(),
            P("tp"),
            P(None, "tp"),
            P(None, "tp"),
            P(),
            P("ep", None, "tp"),
            P("ep", None, "tp"),
            P("ep", None, "tp"),
            P("ep", None),
            P("ep", None),
        ),
        out_specs=(P("ep", "tp"), P("ep", "tp")),
        check_vma=False,
    )
```

```python
import functools

import jax
import jax.numpy as jnp
from jax import lax
from jax.experimental import pallas as pl
from jax.experimental.pallas import tpu as pltpu
from jax.sharding import PartitionSpec as P

TOP = 2
norm_eps = 1e-05
pool_windows = (2, 4, 8, 16)
RIM = 16
MESH = pl.DeviceIdType.MESH
f32 = jnp.float32
bf16 = jnp.bfloat16


def fused(
    ep,
    tp,
    xm_in,
    xe_in,
    gain_m,
    gain_e,
    scale,
    route_rows,
    rw_rows,
    w_in_h,
    w_mix_h,
    gate_h,
    up_h,
    down_h,
    out_m,
    out_e,
    w_in,
    w_mix,
    gate,
    up,
    down,
    xm,
    normed,
    block,
    disp_send,
    slots,
    hid,
    pooled,
    back_send,
    back_recv,
    ext,
    rim_send,
    rim_recv,
    acc,
    as_rows,
    as_cols,
    w_sem,
    sl_s,
    sl_r,
    xm_s,
    xm_r,
    dp_s,
    dp_r,
    rim_s,
    rim_r,
    po_s,
    po_r,
    hi_s,
    hi_r,
    bk_s,
    bk_r,
):
    me_ep = lax.axis_index("ep")
    me_tp = lax.axis_index("tp")
    rows, feat = xm_in.shape
    cap = slots.shape[2]
    chan = out_m.shape[1]
    width = feat * tp
    chunk = min(rows, 128)

    barrier = pltpu.get_barrier_semaphore()
    for d in range(1, tp):
        pl.semaphore_signal(
            barrier, inc=1, device_id={"tp": lax.rem(me_tp + d, tp)}, device_id_type=MESH
        )
    for d in range(1, ep):
        pl.semaphore_signal(
            barrier, inc=1, device_id={"ep": lax.rem(me_ep + d, ep)}, device_id_type=MESH
        )
    pl.semaphore_wait(barrier, tp + ep - 2)

    def tp_copy(ref, s, r, peer):
        return pltpu.make_async_remote_copy(
            src_ref=ref,
            dst_ref=ref,
            send_sem=s,
            recv_sem=r,
            device_id={"tp": peer},
            device_id_type=MESH,
        )

    def ep_copy(src, dst, s, r, d):
        return pltpu.make_async_remote_copy(
            src_ref=src,
            dst_ref=dst,
            send_sem=s,
            recv_sem=r,
            device_id={"ep": lax.rem(me_ep + d, ep)},
            device_id_type=MESH,
        )

    relayed = tp == 4
    col = lax.rem(me_tp, 2)
    row = me_tp // 2
    beside = row * 2 + (1 - col)
    above = (1 - row) * 2 + col
    across = (1 - row) * 2 + (1 - col)

    def send(slot, s, r):
        if relayed:
            tp_copy(slot(me_tp), s(0), r(0), beside).start()
            tp_copy(slot(me_tp), s(1), r(1), above).start()
        else:
            for d in range(1, tp):
                tp_copy(slot(me_tp), s(d - 1), r(d - 1), lax.rem(me_tp + d, tp)).start()

    def relay(slot, s, r, turn):
        if relayed:
            tp_copy(slot(beside), s(0), r(0), beside).wait_recv()
            tp_copy(slot(above), s(1), r(1), above).wait_recv()
            source = (1 - turn) * beside + turn * above
            peer = (1 - turn) * above + turn * beside
            tp_copy(slot(source), s(2), r(2), peer).start()

    def finish(slot, s, r):
        if relayed:
            tp_copy(slot(across), s(2), r(2), across).wait_recv()
        else:
            for d in range(1, tp):
                p = lax.rem(me_tp - d + tp, tp)
                tp_copy(slot(p), s(d - 1), r(d - 1), p).wait_recv()

    def drain(slot, s, r):
        for d in range(1, tp):
            tp_copy(slot(me_tp), s(d - 1), r(d - 1), lax.rem(me_tp + d, tp)).wait_send()

    def mixer_part():
        return lambda p: xm.at[p], lambda j: xm_s.at[j], lambda j: xm_r.at[j]

    def pooled_part():
        return lambda p: pooled.at[p], lambda j: po_s.at[j], lambda j: po_r.at[j]

    def slot_part(k):
        q = ep_from(k)
        return lambda p: slots.at[q, p], lambda j: sl_s.at[k, j], lambda j: sl_r.at[k, j]

    def hidden_part(k):
        q = ep_from(k)
        return lambda p: hid.at[q, p], lambda j: hi_s.at[k, j], lambda j: hi_r.at[k, j]

    def ep_from(d):
        return lax.rem(me_ep - d + ep, ep)

    xm_load = pltpu.make_async_copy(xm_in, xm.at[me_tp], w_sem.at[5])
    xm_load.start()
    xm_load.wait()
    send(*mixer_part())

    loads = [
        pltpu.make_async_copy(h, v, w_sem.at[i])
        for i, (h, v) in enumerate(
            ((w_in_h, w_in), (gate_h, gate), (up_h, up), (w_mix_h, w_mix), (down_h, down))
        )
    ]
    for load in loads:
        load.start()

    t0 = lax.broadcasted_iota(jnp.int32, (rows, rows), 0)
    t1 = lax.broadcasted_iota(jnp.int32, (rows, rows), 1)
    names = lax.broadcasted_iota(jnp.int32, (ep, rows), 0)
    named = [jnp.where(route_rows[j : j + 1, :] == names, 1.0, 0.0) for j in range(TOP)]
    ahead = jnp.dot(
        sum(named).astype(bf16),
        jnp.where(t0 < t1, 1.0, 0.0).astype(bf16),
        preferred_element_type=f32,
    )
    trow = [
        route_rows[j : j + 1, :] * cap
        + jnp.sum(named[j] * ahead, axis=0, keepdims=True).astype(jnp.int32)
        for j in range(TOP)
    ]
    as_rows[...] = jnp.zeros_like(as_rows)
    for j in range(TOP):
        as_rows[j : j + 1, :] = trow[j].astype(f32)
        as_rows[TOP + j : TOP + j + 1, :] = rw_rows[j : j + 1, :]
    as_cols[...] = as_rows[...].T

    def picked_rows(e):
        slot = lax.broadcasted_iota(jnp.int32, (cap, rows), 0) + e * cap
        hit = (slot == trow[0]) | (slot == trow[1])
        pick = jnp.where(hit, 1.0, 0.0).astype(bf16)
        return jnp.dot(pick, xe_in[...], preferred_element_type=f32).astype(bf16)

    def send_rows(d, carry):
        e = lax.rem(me_ep + d, ep)
        disp_send[e] = picked_rows(e)
        ep_copy(disp_send.at[e], slots.at[me_ep, me_tp], dp_s.at[d], dp_r.at[d], d).start()
        return carry

    lax.fori_loop(1, ep, send_rows, 0)
    slots[me_ep, me_tp] = picked_rows(me_ep)
    relay(*mixer_part(), 0)

    def arrive(k):
        q = ep_from(k)
        ep_copy(disp_send.at[q], slots.at[q, me_tp], dp_s.at[k], dp_r.at[k], k).wait_recv()
        send(*slot_part(k))

    arrive(1)

    def pass_slots(k, carry):
        arrive(k)
        relay(*slot_part(k - 1), lax.rem(k, 2))
        return carry

    early = ep // 2
    lax.fori_loop(2, early, pass_slots, 0)

    def norm_rows(parts, gain):
        parts = [v.astype(f32) for v in parts]
        mean = sum(jnp.sum(v, axis=-1, keepdims=True) for v in parts) / width
        parts = [v - mean for v in parts]
        spread = sum(jnp.sum(v * v, axis=-1, keepdims=True) for v in parts) / width
        inv = lax.rsqrt(spread + norm_eps)
        return [
            (v * inv * gain[:, p * feat : (p + 1) * feat]).astype(bf16)
            for p, v in enumerate(parts)
        ]

    finish(*mixer_part())
    loads[0].wait()

    def project(i, carry):
        at = pl.ds(pl.multiple_of(i * chunk, chunk), chunk)
        for p, v in enumerate(norm_rows([xm[p, at, :] for p in range(tp)], gain_m)):
            normed[:, p * feat : (p + 1) * feat] = v
        inner = jnp.dot(normed[...], w_in[...], preferred_element_type=f32).astype(bf16)
        ext[pl.ds(pl.multiple_of(RIM + i * chunk, RIM), chunk), :] = inner.astype(f32)
        return carry

    lax.fori_loop(0, rows // chunk, project, 0)
    rim_send[0] = ext[rows : rows + RIM, :].astype(bf16)
    rim_send[1] = ext[RIM : 2 * RIM, :].astype(bf16)
    up_rim = ep_copy(rim_send.at[0], rim_recv.at[0], rim_s.at[0], rim_r.at[0], 1)
    down_rim = ep_copy(rim_send.at[1], rim_recv.at[1], rim_s.at[1], rim_r.at[1], ep - 1)
    up_rim.start()
    down_rim.start()

    lax.fori_loop(early, ep - 1, pass_slots, 0)

    up_rim.wait_recv()
    down_rim.wait_recv()
    low = rim_recv[0].astype(f32)
    high = rim_recv[1].astype(f32)
    ext[0:RIM, :] = jnp.where(me_ep > 0, low, 0.0)
    ext[RIM + rows : 2 * RIM + rows, :] = jnp.where(me_ep < ep - 1, high, 0.0)

    group_width = chan * tp // len(pool_windows)
    channel = me_tp * chan + lax.broadcasted_iota(jnp.int32, (1, chan), 1)
    seq_len = rows * ep
    for i in range(rows // chunk):
        first = RIM + i * chunk
        position = me_ep * rows + i * chunk + lax.broadcasted_iota(jnp.int32, (chunk, 1), 0)
        running = jnp.zeros((chunk, chan), f32)
        result = jnp.zeros((chunk, chan), f32)
        last = 0
        for g, window in enumerate(pool_windows):
            half = window // 2
            for o in list(range(-half, -last)) + list(range(last, half)):
                running = running + ext[first + o : first + o + chunk, :]
            last = half
            lower = jnp.maximum(position - half, 0)
            upper = jnp.minimum(position + half, seq_len)
            counts = (upper - lower).astype(f32)
            member = (channel >= g * group_width) & (channel < (g + 1) * group_width)
            result = jnp.where(member, running / counts, result)
        values = ext[first : first + chunk, :]
        pooled[me_tp, i * chunk : (i + 1) * chunk, :] = (
            (result - values) * scale[...]
        ).astype(bf16)
    send(*pooled_part())
    pass_slots(ep - 1, 0)
    send(*slot_part(0))

    loads[1].wait()
    loads[2].wait()

    def hidden_step(k):
        q = ep_from(k)
        finish(*slot_part(k))
        for p, v in enumerate(norm_rows([slots[q, p] for p in range(tp)], gain_e)):
            block[:, p * feat : (p + 1) * feat] = v
        x = block[...]
        g = jnp.dot(x, gate[...], preferred_element_type=f32)
        u = jnp.dot(x, up[...], preferred_element_type=f32)
        hid[q, me_tp] = (g / (1.0 + jnp.exp(-g)) * u).astype(bf16)
        send(*hidden_part(k))

    units = hid.shape[3]

    def value_step(k):
        q = ep_from(k)
        finish(*hidden_part(k))
        total = jnp.zeros((cap, out_e.shape[1]), f32)
        for p in range(tp):
            total = total + jnp.dot(
                hid[q, p],
                down[p * units : (p + 1) * units, :],
                preferred_element_type=f32,
            )
        return total.astype(bf16)

    def send_value(k):
        q = ep_from(k)
        back_send[q] = value_step(k)
        ep_copy(back_send.at[q], back_recv.at[me_ep], bk_s.at[k], bk_r.at[k], ep - k).start()

    hidden_step(1)
    relay(*slot_part(ep - 1), ep % 2)
    hidden_step(2)
    relay(*slot_part(0), 1 - ep % 2)
    relay(*pooled_part(), 1)
    relay(*hidden_part(1), 0)

    loads[3].wait()
    finish(*pooled_part())

    def mix_out(i, carry):
        at = pl.ds(pl.multiple_of(i * chunk, chunk), chunk)
        total = jnp.zeros((chunk, chan), f32)
        for p in range(tp):
            total = total + jnp.dot(
                pooled[p, at, :],
                w_mix[p * chan : (p + 1) * chan, :],
                preferred_element_type=f32,
            )
        out_m[at, :] = total.astype(bf16)
        return carry

    lax.fori_loop(0, rows // chunk, mix_out, 0)
    loads[4].wait()

    def expert(k, carry):
        hidden_step(k)
        relay(*hidden_part(k - 1), lax.rem(k, 2))
        send_value(k - 2)
        return carry

    lax.fori_loop(3, ep, expert, 0)
    hidden_step(0)
    relay(*hidden_part(ep - 1), ep % 2)
    send_value(ep - 2)
    relay(*hidden_part(0), 1 - ep % 2)
    send_value(ep - 1)

    def combine(e):
        slot = lax.broadcasted_iota(jnp.int32, (rows, cap), 1) + e * cap
        weight = jnp.zeros((rows, cap), f32)
        for j in range(TOP):
            own_slot = as_cols[:, j : j + 1].astype(jnp.int32)
            weight = weight + jnp.where(slot == own_slot, as_cols[:, TOP + j : TOP + j + 1], 0.0)
        coarse = weight.astype(bf16)
        fine = (weight - coarse.astype(f32)).astype(bf16)
        v = back_recv[e]
        return jnp.dot(coarse, v, preferred_element_type=f32) + jnp.dot(
            fine, v, preferred_element_type=f32
        )

    acc[...] = jnp.zeros_like(acc)

    def gather_value(k, carry):
        e = lax.rem(me_ep + k, ep)
        ep_copy(back_send.at[e], back_recv.at[e], bk_s.at[k], bk_r.at[k], k).wait_recv()
        acc[...] += combine(e)
        return carry

    lax.fori_loop(1, ep - 2, gather_value, 0)
    back_recv[me_ep] = value_step(0)
    acc[...] += combine(me_ep)
    lax.fori_loop(ep - 2, ep, gather_value, 0)
    out_e[...] = acc[...].astype(bf16)

    drain(*mixer_part())
    drain(*pooled_part())
    up_rim.wait_send()
    down_rim.wait_send()

    def drain_ep(k, carry):
        e = lax.rem(me_ep + k, ep)
        q = ep_from(k)
        ep_copy(disp_send.at[e], slots.at[me_ep, me_tp], dp_s.at[k], dp_r.at[k], k).wait_send()
        ep_copy(back_send.at[q], back_recv.at[me_ep], bk_s.at[k], bk_r.at[k], ep - k).wait_send()
        return carry

    lax.fori_loop(1, ep, drain_ep, 0)

    def drain_tp(k, carry):
        drain(*slot_part(k))
        drain(*hidden_part(k))
        return carry

    lax.fori_loop(0, ep, drain_tp, 0)


def on_device(
    mixer_rows,
    expert_rows,
    mixer_gain,
    pool_scale,
    w_in,
    w_mix_out,
    expert_gain,
    expert_gate,
    expert_up,
    expert_down,
    routes,
    route_weight,
    *,
    ep,
    tp,
):
    rows, feat = mixer_rows.shape
    width = feat * tp
    cap = (3 * TOP * rows + 2 * ep - 1) // (2 * ep)
    chan = w_in.shape[1]
    units = expert_gate.shape[2]
    vmem = pl.BlockSpec(memory_space=pltpu.VMEM)
    hbm = pl.BlockSpec(memory_space=pl.ANY)
    dma = pltpu.SemaphoreType.DMA
    return pl.pallas_call(
        functools.partial(fused, ep, tp),
        out_shape=(
            jax.ShapeDtypeStruct((rows, w_mix_out.shape[1]), bf16),
            jax.ShapeDtypeStruct((rows, expert_down.shape[2]), bf16),
        ),
        in_specs=[vmem] * 7 + [hbm] * 5,
        out_specs=(vmem, vmem),
        scratch_shapes=[
            pltpu.VMEM(w_in.shape, bf16),
            pltpu.VMEM(w_mix_out.shape, bf16),
            pltpu.VMEM(expert_gate.shape[1:], bf16),
            pltpu.VMEM(expert_up.shape[1:], bf16),
            pltpu.VMEM(expert_down.shape[1:], bf16),
            pltpu.VMEM((tp, rows, feat), bf16),
            pltpu.VMEM((min(rows, 128), width), bf16),
            pltpu.VMEM((cap, width), bf16),
            pltpu.VMEM((ep, cap, feat), bf16),
            pltpu.VMEM((ep, tp, cap, feat), bf16),
            pltpu.VMEM((ep, tp, cap, units), bf16),
            pltpu.VMEM((tp, rows, chan), bf16),
            pltpu.VMEM((ep, cap, expert_down.shape[2]), bf16),
            pltpu.VMEM((ep, cap, expert_down.shape[2]), bf16),
            pltpu.VMEM((rows + 2 * RIM, chan), f32),
            pltpu.VMEM((2, RIM, chan), bf16),
            pltpu.VMEM((2, RIM, chan), bf16),
            pltpu.VMEM((rows, expert_down.shape[2]), f32),
            pltpu.VMEM((8, rows), f32),
            pltpu.VMEM((rows, 8), f32),
            dma((6,)),
            dma((ep, tp - 1)),
            dma((ep, tp - 1)),
            dma((tp - 1,)),
            dma((tp - 1,)),
            dma((ep,)),
            dma((ep,)),
            dma((2,)),
            dma((2,)),
            dma((tp - 1,)),
            dma((tp - 1,)),
            dma((ep, tp - 1)),
            dma((ep, tp - 1)),
            dma((ep,)),
            dma((ep,)),
        ],
        compiler_params=pltpu.CompilerParams(
            collective_id=0, has_side_effects=True, vmem_limit_bytes=62 * 1024 * 1024
        ),
    )(
        mixer_rows,
        expert_rows,
        mixer_gain.reshape(1, width),
        expert_gain.reshape(1, width),
        pool_scale.reshape(1, chan),
        routes.T,
        route_weight.T,
        w_in,
        w_mix_out,
        expert_gate.reshape(expert_gate.shape[1:]),
        expert_up.reshape(expert_up.shape[1:]),
        expert_down.reshape(expert_down.shape[1:]),
    )


def solution(mesh):
    return jax.shard_map(
        functools.partial(on_device, ep=mesh.shape["ep"], tp=mesh.shape["tp"]),
        mesh=mesh,
        in_specs=(
            P("ep", "tp"),
            P("ep", "tp"),
            P(),
            P("tp"),
            P(None, "tp"),
            P(None, "tp"),
            P(),
            P("ep", None, "tp"),
            P("ep", None, "tp"),
            P("ep", None, "tp"),
            P("ep", None),
            P("ep", None),
        ),
        out_specs=(P("ep", "tp"), P("ep", "tp")),
        check_vma=False,
    )
```
